256 devices in a mesh: sp: 16 (over y, x), tp: 16 (over z, core).
Axes of the slice: x: 4, y: 4, z: 8, core: 2. Of those that a mesh axis runs over, the one named last changes fastest.
Arguments:
- gate_b: bfloat16 [8192, 1024], P('sp', 'tp'), may hold values from -6 to 6
- gate_c: bfloat16 [8192, 1024], P('sp', 'tp'), may hold values from -6 to 6
- values_in: bfloat16 [8192, 1024], P('sp', 'tp'), may hold values from -6 to 6
- conv_w: bfloat16 [3, 1024], P(None, 'tp'), may hold values from -3.5 to 3.5
- documents: int32 [8192], P('sp'), may hold values from 0 to 8, never falling along the last dimension, each value on 1 to 4096 neighbouring positions
- w_out: bfloat16 [1024, 2048], replicated, may hold values from -0.1875 to 0.1875
- resid: bfloat16 [8192, 2048], P(('sp', 'tp')), may hold values from -6 to 6
- norm_gain: bfloat16 [2048], replicated, may hold values from 0.099609375 to 1.8984375
- route_ids: int32 [8192, 2], P(('sp', 'tp')), may hold values from 0 to 15, all different within a row; in each aligned block of 32 rows (0 to 31, 32 to 63, ...) at most 8 rows name the same one
- route_weight: float32 [8192, 2], P(('sp', 'tp')), may hold values from 0.2 to 1
- w_gate: bfloat16 [16, 2048, 7168], P('sp', None, 'tp'), may hold values from -0.125 to 0.125
- w_up: bfloat16 [16, 2048, 7168], P('sp', None, 'tp'), may hold values from -0.125 to 0.125
- w_down: bfloat16 [16, 7168, 2048], P('sp', 'tp'), may hold values from -0.0625 to 0.0625
Outputs:
- layer_out: bfloat16 [8192, 2048], P(('sp', 'tp'))
The draws below stay inside these ranges and needn't reach their ends.
Inputs may be any that keep to these rules, and one draw needn't show every extreme that they name: `route_ids`: each token names two different experts; in the rows of one device no expert is named by more than 8 rows, a bound that some block reaches. `documents`: document numbers never fall along the positions; a document has at most 8192 // 2 positions.
All inputs are finite; a program needn't handle non-finite values.
Results may differ from the reference program's by a relative error of at most 0.018.
Values may be sent and summed in bfloat16 or wider, within the bound.
A program may use at most 128 MiB of HBM per device.

```python
import math
import jax
import jax.numpy as jnp
import numpy as np
from jax import lax

D = 2048
CH = 1024
FF_E = 7168
KW = 3
TOKENS = 8192
ROWS = 32
EXPERTS = 16
CAP = 8
N_SP = 16
N_TP = 16


def shard_levels(key, extent, cuts, least, high):
    gain, own = 1.0, jax.random.fold_in(key, 6)
    for dim, shards_of in cuts:
        draws = jnp.exp(jax.random.uniform(jax.random.fold_in(own, dim), (shards_of,), jnp.float32, least / len(cuts), high / len(cuts)))
        gain = gain * jnp.repeat(draws, extent[dim] // shards_of).reshape([-1 if axis == dim else 1 for axis in range(len(extent))])
    return gain


def profile(number_of, total, bound, skew):
    portions = [(1 << 20) // math.isqrt(rank ** skew) + 1 for rank in range(2, number_of + 1)]
    surplus, counts = total - bound - (number_of - 1), [1] * (number_of - 1)
    while surplus > 0:
        candidates = [i for i in range(number_of - 1) if counts[i] < bound]
        mass, left = sum([portions[i] for i in candidates]), surplus
        for i in candidates:
            addition = min(bound - counts[i], max(1, left * portions[i] // mass), surplus)
            counts[i] = counts[i] + addition
            surplus = surplus - addition
    return np.array([bound] + counts)


def ragged_sizes(stream_key, amount, total, limit, skew):
    if amount == 2:
        one = jax.random.randint(stream_key, (), max(1, total - limit), min(limit, total - 1) + 1)
        return jnp.stack([one, total - one])
    lengths = jnp.asarray(profile(amount, total, limit, skew), jnp.int32)
    couples = (amount - 1) // 2
    giver, sink = lengths[1:1 + 2 * couples:2], lengths[2:2 + 2 * couples:2]
    slack = jnp.minimum(giver - 1, limit - sink)
    moved = jax.random.randint(jax.random.fold_in(stream_key, 1), (couples,), 0, 1 << 20) % (slack + 1)
    lengths = lengths.at[1:1 + 2 * couples:2].set(giver - moved).at[2:2 + 2 * couples:2].set(sink + moved)
    return lengths[jax.random.permutation(jax.random.fold_in(stream_key, 2), amount)]


def assign_block(own_key, own, number, rows, number_of, top, limit, skew):
    order = jax.random.permutation(own_key, number_of)
    crowded, common = shares(number_of, rows * top, limit, skew, True), shares(number_of, rows * top, limit, skew, False)
    places = jnp.arange(number_of)

    def named(lengths, rotation):
        used = int((lengths > 0).sum())
        fixed = max(1, used // 4)
        shifted = fixed + (places - fixed + rotation * (used - fixed)) % max(1, number_of - fixed)
        return jnp.zeros((number_of,), jnp.int32).at[order[jnp.where(places < fixed, places, shifted)]].set(jnp.asarray(lengths, jnp.int32))

    lengths = jnp.where(number % 4 == 0, named(crowded, number // 4), named(common, number - number // 4 - 1))
    mixed = jax.random.permutation(jax.random.fold_in(own, 3), number_of)
    giver, receiver = mixed[0:number_of // 2 * 2:2], mixed[1:number_of // 2 * 2:2]
    slack = jnp.minimum(lengths[giver] - 1, limit - lengths[receiver]) // 2
    slack = jnp.where((giver == order[0]) | (receiver == order[0]) | (lengths[receiver] == 0), 0, jnp.maximum(slack, 0))
    shifted = jax.random.randint(jax.random.fold_in(own, 4), (number_of // 2,), 0, 1 << 20) % (slack + 1)
    lengths = lengths.at[giver].add(-shifted).at[receiver].add(shifted)
    items = jnp.searchsorted(jnp.cumsum(lengths), jnp.arange(rows * top), side="right").astype(jnp.int32)
    listing = items.reshape(top, rows).T
    listing = listing[jax.random.permutation(jax.random.fold_in(own, 1), rows)]
    rotation = jax.random.randint(jax.random.fold_in(own, 2), (rows, 1), 0, top)
    return jnp.take_along_axis(listing, (jnp.arange(top)[None, :] + rotation) % top, axis=1)


def shares(count, total, bound, lean, full):
    loads = [(1 << 20) // math.isqrt(grade ** lean) + 1 for grade in range(1, count + 1)]
    largest = bound if full else min(bound, max(-(-total // count), total * loads[0] // sum(loads)))
    least = 1 if total - largest >= count - 1 else 0
    counts, spare = [largest] + [least] * (count - 1), total - largest - least * (count - 1)
    while spare > 0:
        movable = [i for i in range(1, count) if counts[i] < largest] or [i for i in range(1, count) if counts[i] < bound]
        mass, remaining = sum([loads[i] for i in movable]), spare
        for i in movable:
            addition = min(bound - counts[i], max(1, remaining * loads[i] // mass), spare)
            counts[i] = counts[i] + addition
            spare = spare - addition
    return np.array(counts)


def centred(stream_key, dims, deviation, most, cuts=(), held_as=jnp.bfloat16):
    factor_of = shard_levels(stream_key, dims, cuts, -0.22, 0.18) if cuts else 1.0
    result = jax.random.normal(stream_key, dims, jnp.float32) * deviation * factor_of
    return jnp.minimum(jnp.maximum(result, -most), most).astype(held_as)


def setup_inputs(seed: int = 0) -> dict:
    arg_keys = jax.random.split(jax.random.key(seed), 14)
    gate_b = centred(arg_keys[0], (TOKENS, CH), 1.0, 6.0, ((0, 16), (1, 16)))
    gate_c = centred(arg_keys[1], (TOKENS, CH), 1.0, 6.0, ((0, 16), (1, 16)))
    values_in = centred(arg_keys[2], (TOKENS, CH), 1.0, 6.0, ((0, 16), (1, 16)))
    conv_w = centred(arg_keys[3], (KW, CH), KW ** -0.5, 3.5, ((1, 16),))
    documents = jnp.searchsorted(jnp.cumsum(ragged_sizes(arg_keys[4], N_SP // 2 + 1, TOKENS, TOKENS // 2, 1)), jnp.arange(TOKENS), side="right").astype(jnp.int32)
    w_out = centred(arg_keys[5], (CH, D), CH ** -0.5, 0.1875)
    resid = centred(arg_keys[6], (TOKENS, D), 1.0, 6.0, ((0, 256),))
    norm_gain = jnp.clip(1.0 + 0.18 * jax.random.normal(arg_keys[7], (D,), jnp.float32), 0.099609375, 1.8984375).astype(jnp.bfloat16)
    route_ids_keys = jax.random.split(jax.random.fold_in(arg_keys[8], 1), TOKENS // ROWS)
    route_ids_turns = jax.random.permutation(jax.random.fold_in(arg_keys[8], 3), TOKENS // ROWS)
    route_ids = jax.vmap(lambda own, number: assign_block(jax.random.fold_in(arg_keys[8], 2), own, number, ROWS, EXPERTS, 2, CAP, 2))(route_ids_keys, route_ids_turns).reshape((TOKENS, 2))
    route_weight = jnp.clip(0.2 + 0.8 * jax.random.uniform(arg_keys[9], (TOKENS, 2), jnp.float32) ** shard_levels(arg_keys[9], (TOKENS, 2), ((0, 256),), -0.2, 0.2), 0.2, 1.0)
    w_gate = centred(arg_keys[10], (EXPERTS, D, FF_E), D ** -0.5, 0.125, ((0, 16), (2, 16)))
    w_up = centred(arg_keys[11], (EXPERTS, D, FF_E), D ** -0.5, 0.125, ((0, 16), (2, 16)))
    w_down = centred(arg_keys[12], (EXPERTS, FF_E, D), FF_E ** -0.5, 0.0625, ((0, 16), (1, 16)))
    return {"gate_b": gate_b, "gate_c": gate_c, "values_in": values_in, "conv_w": conv_w, "documents": documents, "w_out": w_out, "resid": resid, "norm_gain": norm_gain, "route_ids": route_ids, "route_weight": route_weight, "w_gate": w_gate, "w_up": w_up, "w_down": w_down}


def reference(gate_b, gate_c, values_in, conv_w, documents, w_out, resid, norm_gain, route_ids, route_weight, w_gate, w_up, w_down):
    product = gate_c.astype(jnp.float32) * values_in.astype(jnp.float32)
    padded = jnp.concatenate([jnp.zeros((2, CH), jnp.float32), product], axis=0)
    padded_docs = jnp.concatenate([jnp.full((2,), -1, jnp.int32), documents], axis=0)
    kernel_taps = conv_w.astype(jnp.float32)
    near_mask = (padded_docs[1:-1] == documents).astype(jnp.float32)[:, None]
    far_mask = (padded_docs[:-2] == documents).astype(jnp.float32)[:, None]
    convolved = kernel_taps[2] * product + kernel_taps[1] * padded[1:-1] * near_mask + kernel_taps[0] * padded[:-2] * far_mask
    mixed_rows = (gate_b.astype(jnp.float32) * convolved).astype(jnp.bfloat16)
    projected = jnp.dot(mixed_rows, w_out, preferred_element_type=jnp.float32)
    hidden_state = (resid.astype(jnp.float32) + projected).astype(jnp.bfloat16)
    state_wide = hidden_state.astype(jnp.float32)
    normed = (state_wide * lax.rsqrt(lax.optimization_barrier(jnp.mean(state_wide * state_wide, axis=-1, keepdims=True)) + 1e-06) * norm_gain.astype(jnp.float32)).astype(jnp.bfloat16)
    blocks = TOKENS // ROWS
    block_ids = route_ids.reshape(blocks, 2 * ROWS)
    one_hot = (block_ids[:, :, None] == jnp.arange(EXPERTS, dtype=jnp.int32)[None, None, :]).astype(jnp.int32)
    rank_in = lax.optimization_barrier(jnp.sum((jnp.cumsum(one_hot, axis=1) - one_hot) * one_hot, axis=2))
    per_expert = blocks * CAP
    block_index = jnp.arange(blocks, dtype=jnp.int32)[:, None]
    flat_slot = (block_ids * per_expert + block_index * CAP + rank_in).astype(jnp.int32)
    token_index = (block_index * ROWS + jnp.arange(2 * ROWS, dtype=jnp.int32)[None, :] // 2).astype(jnp.int32)
    slot_table = jnp.full((EXPERTS * per_expert,), TOKENS, jnp.int32).at[flat_slot.reshape(-1)].set(token_index.reshape(-1))
    padded_rows = jnp.concatenate([normed, jnp.zeros((1, D), jnp.bfloat16)], axis=0)

    def serve_expert(operands):
        slot_rows, gate_weight, up_weight, down_weight = operands
        chosen = padded_rows[slot_rows]
        gate_part = jnp.dot(chosen, gate_weight, preferred_element_type=jnp.float32)
        up_part = jnp.dot(chosen, up_weight, preferred_element_type=jnp.float32)
        activated = (jax.nn.silu(gate_part) * up_part).astype(jnp.bfloat16)
        pieces = jnp.einsum('snf,nfd->snd', activated.reshape(per_expert, N_TP, FF_E // N_TP).astype(jnp.float32), down_weight.reshape(N_TP, FF_E // N_TP, D).astype(jnp.float32))
        rounded = lax.optimization_barrier(pieces.astype(jnp.bfloat16))
        return lax.optimization_barrier(jnp.sum(rounded.astype(jnp.float32), axis=1)).astype(jnp.bfloat16)
    expert_out = lax.map(serve_expert, (slot_table.reshape(EXPERTS, per_expert), w_gate, w_up, w_down))
    picked = expert_out.reshape(EXPERTS * per_expert, D)[flat_slot.reshape(TOKENS, 2)]
    combined = lax.optimization_barrier(jnp.sum(route_weight[:, :, None].astype(jnp.float32) * picked.astype(jnp.float32), axis=1))
    return (hidden_state.astype(jnp.float32) + combined).astype(jnp.bfloat16)
```

```python
import functools

import jax
import jax.numpy as jnp
from jax import lax
from jax.experimental import pallas as pl
from jax.experimental.pallas import tpu as pltpu
from jax.sharding import PartitionSpec as P

MESH = pl.DeviceIdType.MESH
F32 = jnp.float32
BF16 = jnp.bfloat16
NT = (((1,), (1,)), ((), ()))


def kernel(
    S, T, G,
    gb_hbm, gc_hbm, v_hbm, taps_ref, docs_ref, wout_hbm, resid_hbm, gain_ref, ids_ref, rw_ref,
    wg_hbm, wu_hbm, wd_hbm,
    out_ref,
    gb, gc, vin, wout, resid, wg, wu, wd,
    halo_out, halo_in, mix, pieces, dsp, X, Y, YS, YP, R, OUT, RET, hid,
    in_sem, halo_sem, a2a_s, a2a_r, dsp_s, dsp_r, ag_s, ag_r, xd_s, xd_r, yd_s, yd_r,
    rs_s, rs_r, ret_s, ret_r,
):
    sp = lax.axis_index("sp")
    tp = lax.axis_index("tp")
    Z = T // 2
    H = Z // 2
    z = tp // 2
    c = lax.rem(tp, 2)
    mate = tp + 1 - 2 * c
    rows, D = resid.shape
    chl, seq = gb.shape
    cap = dsp.shape[1]
    B = S * cap
    GR = B // G
    SG = S // G
    half = G // 2

    def loc(i, src, dst):
        return pltpu.make_async_copy(src, dst, in_sem.at[i])

    loads = [
        loc(0, gc_hbm, gc), loc(1, v_hbm, vin), loc(2, gb_hbm, gb), loc(3, wout_hbm, wout),
        loc(4, resid_hbm, resid), loc(5, wg_hbm, wg), loc(6, wu_hbm, wu), loc(7, wd_hbm, wd),
    ]
    for copy in loads:
        copy.start()

    barrier = pltpu.get_barrier_semaphore()

    def greet_tp(k, _):
        pl.semaphore_signal(barrier, inc=1, device_id=(sp, lax.rem(tp + k, T)), device_id_type=MESH)
        return 0

    def greet_sp(k, _):
        pl.semaphore_signal(barrier, inc=1, device_id=(lax.rem(sp + k, S), tp), device_id_type=MESH)
        return 0

    lax.fori_loop(1, T, greet_tp, 0)
    lax.fori_loop(1, S, greet_sp, 0)

    def rdma(src, dst, ssem, rsem, dev):
        return pltpu.make_async_remote_copy(
            src_ref=src, dst_ref=dst, send_sem=ssem, recv_sem=rsem, device_id=dev, device_id_type=MESH
        )

    loads[0].wait()
    loads[1].wait()
    product = gc[...].astype(F32) * vin[...].astype(F32)
    docs = docs_ref[...]
    halo_out[0:chl, :] = product[:, seq - 128 :]
    halo_out[chl : chl + 8, :] = jnp.broadcast_to(docs[:, seq - 128 :].astype(F32), (8, 128))

    pl.semaphore_wait(barrier, (T - 1) + (S - 1))

    halo = rdma(halo_out, halo_in, halo_sem.at[0], halo_sem.at[1], (lax.rem(sp + 1, S), tp))
    halo.start()

    lane = lax.broadcasted_iota(jnp.int32, (B, 128), 1)
    slot = lax.broadcasted_iota(jnp.int32, (B, 128), 0)
    ids = jnp.concatenate([ids_ref[...], jnp.full((2, 128 - rows), -1, jnp.int32)], axis=1)
    hit0 = ids[0:1, :] == slot // cap
    hit1 = ids[1:2, :] == slot // cap
    hits = jnp.where(hit0 | hit1, 1.0, 0.0).astype(BF16)
    below = jnp.where(
        lax.broadcasted_iota(jnp.int32, (128, 128), 0) < lax.broadcasted_iota(jnp.int32, (128, 128), 1), 1.0, 0.0
    ).astype(BF16)
    rank = jnp.dot(hits, below, preferred_element_type=F32)
    mine = rank == lax.rem(slot, cap).astype(F32)
    place0 = jnp.where(hit0 & mine, 1.0, 0.0)
    place1 = jnp.where(hit1 & mine, 1.0, 0.0)
    place = (place0 + place1).astype(BF16)

    eye = jnp.where(
        lax.broadcasted_iota(jnp.int32, (chl, chl), 0) == lax.broadcasted_iota(jnp.int32, (chl, chl), 1), 1.0, 0.0
    ).astype(BF16)
    taps = lax.dot_general(eye, taps_ref[...], NT, preferred_element_type=F32)
    loads[2].wait()

    halo.wait()
    before = jnp.concatenate([halo_in[0:chl, :], product], axis=1)
    old_docs = jnp.where(sp > 0, halo_in[chl : chl + 1, :].astype(jnp.int32), -1)
    all_docs = jnp.concatenate([old_docs, docs], axis=1)
    prev1 = pltpu.roll(before, 1, 1)[:, 128:]
    prev2 = pltpu.roll(before, 2, 1)[:, 128:]
    wide_docs = jnp.broadcast_to(all_docs, (8, 128 + seq))
    near = (pltpu.roll(wide_docs, 1, 1)[0:1, 128:] == docs).astype(F32)
    far = (pltpu.roll(wide_docs, 2, 1)[0:1, 128:] == docs).astype(F32)
    conv = taps[:, 2:3] * product + taps[:, 1:2] * prev1 * near + taps[:, 0:1] * prev2 * far
    mixed = (gb[...].astype(F32) * conv).astype(BF16).astype(F32)
    odd = c == 1
    spread = jnp.concatenate([jnp.where(odd, 0.0, mixed), jnp.where(odd, mixed, 0.0)], axis=0)
    mix[...] = spread.T.astype(BF16).reshape(T, rows, 2 * chl)

    def send_piece(k, _):
        p = lax.rem(tp + k, T)
        rdma(mix.at[p], pieces.at[tp], a2a_s.at[p], a2a_r.at[tp], (sp, p)).start()
        return 0

    lax.fori_loop(1, T, send_piece, 0)
    pieces[tp] = mix[tp]

    def take_piece(k, _):
        p = lax.rem(tp + k, T)
        rdma(mix.at[p], pieces.at[p], a2a_s.at[p], a2a_r.at[p], (sp, p)).wait_recv()
        return 0

    loads[3].wait()
    loads[4].wait()
    lax.fori_loop(1, T, take_piece, 0)
    token_rows = jnp.concatenate([pieces[2 * k] + pieces[2 * k + 1] for k in range(Z)], axis=1)
    projected = jnp.dot(token_rows, wout[...], preferred_element_type=F32)
    hidden = (resid[...].astype(F32) + projected).astype(BF16)
    hid[...] = hidden
    wide = hidden.astype(F32)
    normed = (
        wide * lax.rsqrt(jnp.mean(wide * wide, axis=-1, keepdims=True) + 1e-06) * gain_ref[...].astype(F32)
    ).astype(BF16)
    dispatch = jnp.dot(place[:, 0:rows], normed, preferred_element_type=F32).astype(BF16)
    dsp[...] = dispatch.reshape(S, cap, D)

    def slots(ref, s):
        return ref.at[pl.ds(pl.multiple_of(s * cap, cap), cap)]

    def send_rows(k, _):
        e = lax.rem(sp + k, S)
        rdma(dsp.at[e], slots(X.at[tp], sp), dsp_s.at[e], dsp_r.at[sp], (e, tp)).start()
        return 0

    lax.fori_loop(1, S, send_rows, 0)
    own = pltpu.make_async_copy(dsp.at[sp], slots(X.at[tp], sp), dsp_r.at[sp])
    own.start()

    def part(ref, b, g):
        return ref.at[b, pl.ds(pl.multiple_of(g * GR, GR), GR)]

    def up_ok(d, g):
        return (d < H) | ((d == H) & (g < half))

    def down_ok(d, g):
        return (d < H) | ((d == H) & (g >= half))

    above = (sp, 2 * lax.rem(z + 1, Z) + c)
    beneath = (sp, 2 * lax.rem(z + Z - 1, Z) + c)
    other = (sp, mate)

    def ring_gather(way, d, g, b):
        r = part(X, b, g)
        return rdma(r, r, ag_s.at[way, d - 1, g], ag_r.at[way, d - 1, g], above if way == 0 else beneath)

    def share(zz, g):
        r = part(X, 2 * zz + c, g)
        return rdma(r, r, xd_s.at[zz, g], xd_r.at[zz, g], other)

    def take_share(zz, g):
        r = part(X, 2 * zz + 1 - c, g)
        rdma(r, r, xd_s.at[zz, g], xd_r.at[zz, g], other).wait_recv()

    for g in range(G):
        for s in range(g * SG, (g + 1) * SG):
            pltpu.make_async_copy(dsp.at[s], slots(X.at[tp], s), dsp_r.at[s]).wait()
        if 1 < H or g < half:
            ring_gather(0, 1, g, tp).start()
        if 1 < H or g >= half:
            ring_gather(1, 1, g, tp).start()
        share(z, g).start()
    for k in range(5, 8):
        loads[k].wait()

    def expert(d, j):
        @pl.when((d > 0) | (j < 2))
        def _():
            zz = lax.rem(z + Z + jnp.where(j < 2, d, -d), Z)
            core = lax.rem(c + j + jnp.where(d > 0, 1, 0), 2)
            theirs = core != c

            @pl.when(theirs)
            def _():
                for g in range(G):
                    take_share(zz, g)

            x = X[2 * zz + core]
            gate = lax.dot_general(x, wg[...], NT, preferred_element_type=F32)
            up = lax.dot_general(x, wu[...], NT, preferred_element_type=F32)
            act = (gate * jax.nn.sigmoid(gate) * up).astype(BF16)
            y = jnp.dot(act, wd[...], preferred_element_type=F32).astype(BF16)

            @pl.when(theirs)
            def _():
                YS[zz] = y
                rdma(YS.at[zz], YP.at[zz], yd_s.at[zz], yd_r.at[zz], other).start()

            @pl.when(jnp.logical_not(theirs))
            def _():
                Y[zz] = y

    def gather_step(d, g):
        @pl.when(up_ok(d, g))
        def _():
            zz = lax.rem(z + Z - d, Z)
            ring_gather(0, d, g, 2 * zz + c).wait_recv()

            @pl.when(up_ok(d + 1, g))
            def _():
                ring_gather(0, d + 1, g, 2 * zz + c).start()

            share(zz, g).start()

        @pl.when(down_ok(d, g))
        def _():
            zz = lax.rem(z + d, Z)
            ring_gather(1, d, g, 2 * zz + c).wait_recv()

            @pl.when(down_ok(d + 1, g))
            def _():
                ring_gather(1, d + 1, g, 2 * zz + c).start()

            share(zz, g).start()

    def ring_sum(way, d, g, zz):
        return rdma(part(Y, zz, g), part(R.at[way], d - 1, g), rs_s.at[way, d - 1, g], rs_r.at[way, d - 1, g],
                    above if way == 0 else beneath)

    def take_sum(way, d, g, zz):
        rdma(part(Y, zz, g), part(R.at[way], d, g), rs_s.at[way, d, g], rs_r.at[way, d, g],
             above if way == 0 else beneath).wait_recv()

    def take_y(zz):
        rdma(YS.at[zz], YP.at[zz], yd_s.at[zz], yd_r.at[zz], other).wait_recv()

    def rows_of(g):
        return pl.ds(pl.multiple_of(g * GR, GR), GR)

    def sum_start(way, d, g, fresh):
        zz = lax.rem(z + d, Z) if way == 0 else lax.rem(z + Z - d, Z)
        total = Y[zz, rows_of(g)].astype(F32) + YP[zz, rows_of(g)].astype(F32)
        if not fresh:
            take_sum(way, d, g, zz)
            total = total + R[way, d, rows_of(g)].astype(F32)
        Y[zz, rows_of(g)] = total.astype(BF16)
        ring_sum(way, d, g, zz).start()

    def early_sums():
        if H > 1:
            take_y(lax.rem(z + H - 1, Z))
            take_y(lax.rem(z + Z - (H - 1), Z))
            for g in range(half):
                sum_start(0, H - 1, half + g, True)
                sum_start(1, H - 1, g, True)

    steps = H * G

    def step(i, _):
        d = i // G
        j = lax.rem(i, G)

        @pl.when(i == steps)
        def _():
            early_sums()

        @pl.when(j < 4)
        def _():
            expert(d, j)

        if G < 4:
            for extra in range(G, 4):
                @pl.when((j == G - 1) & (i < steps))
                def _():
                    expert(d, extra)

        @pl.when(i < steps)
        def _():
            gather_step(d + 1, j)

        return 0

    lax.fori_loop(0, steps + 2, step, 0)

    take_y(lax.rem(z + H, Z))
    for g in range(half):
        sum_start(0, H, g, True)
        sum_start(1, H, half + g, True)
    if H > 1:
        for g in range(half):
            sum_start(0, H - 1, g, False)
            sum_start(1, H - 1, half + g, False)

    def sum_step(i, _):
        d = H - 2 - i // G
        g = lax.rem(i, G)

        @pl.when(g == 0)
        def _():
            take_y(lax.rem(z + d, Z))
            take_y(lax.rem(z + Z - d, Z))

        sum_start(0, d, g, False)
        sum_start(1, d, g, False)
        return 0

    if H > 2:
        lax.fori_loop(0, (H - 2) * G, sum_step, 0)

    take_y(z)
    for g in range(G):
        lo, hi = g * GR, (g + 1) * GR
        total = Y[z, lo:hi].astype(F32) + YP[z, lo:hi].astype(F32)
        if 1 < H or g < half:
            take_sum(0, 0, g, z)
            total = total + R[0, 0, lo:hi].astype(F32)
        if 1 < H or g >= half:
            take_sum(1, 0, g, z)
            total = total + R[1, 0, lo:hi].astype(F32)
        OUT[g * SG : (g + 1) * SG] = total.astype(BF16).reshape(SG, cap, D)
        for s in range(g * SG, (g + 1) * SG):
            @pl.when(sp != s)
            def _():
                rdma(OUT.at[s], slots(RET, sp), ret_s.at[s], ret_r.at[sp], (s, tp)).start()

            @pl.when(sp == s)
            def _():
                pltpu.make_async_copy(OUT.at[s], slots(RET, s), ret_r.at[s]).start()

    pick0 = place0.T[0:rows].astype(BF16)
    pick1 = place1.T[0:rows].astype(BF16)
    rw = jnp.concatenate([rw_ref[...], jnp.zeros((2, 128 - rows), F32)], axis=1)
    w0 = jnp.broadcast_to(rw[0:1], (128, 128)).T[0:rows, 0:1]
    w1 = jnp.broadcast_to(rw[1:2], (128, 128)).T[0:rows, 0:1]

    for s in range(S):
        pltpu.make_async_copy(OUT.at[s], slots(RET, s), ret_r.at[s]).wait()
    back = RET[...]
    got0 = jnp.dot(pick0, back, preferred_element_type=F32)
    got1 = jnp.dot(pick1, back, preferred_element_type=F32)
    out_ref[...] = (hid[...].astype(F32) + (w0 * got0 + w1 * got1)).astype(BF16)

    halo_done = 0
    del halo_done

    def sent_piece(k, _):
        p = lax.rem(tp + k, T)
        rdma(mix.at[p], pieces.at[p], a2a_s.at[p], a2a_r.at[p], (sp, p)).wait_send()
        return 0

    def sent_rows(k, _):
        e = lax.rem(sp + k, S)
        rdma(dsp.at[e], slots(X.at[tp], e), dsp_s.at[e], dsp_r.at[e], (e, tp)).wait_send()
        rdma(OUT.at[e], slots(RET, e), ret_s.at[e], ret_r.at[e], (e, tp)).wait_send()
        return 0

    lax.fori_loop(1, T, sent_piece, 0)
    lax.fori_loop(1, S, sent_rows, 0)
    for way, ok in ((0, up_ok), (1, down_ok)):
        def sent_ring(i, _):
            d = i // G + 1
            g = lax.rem(i, G)

            @pl.when(ok(d, g))
            def _():
                ring_gather(way, d, g, tp).wait_send()
                ring_sum(way, d, g, z).wait_send()

            return 0

        lax.fori_loop(0, steps, sent_ring, 0)

    def sent_share(i, _):
        share(i // G, lax.rem(i, G)).wait_send()
        return 0

    def sent_y(zz, _):
        rdma(YS.at[zz], YP.at[zz], yd_s.at[zz], yd_r.at[zz], other).wait_send()
        return 0

    lax.fori_loop(0, Z * G, sent_share, 0)
    lax.fori_loop(0, Z, sent_y, 0)


def local(
    gate_b, gate_c, values_in, conv_w, documents, w_out, resid, norm_gain, route_ids, route_weight,
    w_gate, w_up, w_down,
):
    S, T = lax.axis_size("sp"), lax.axis_size("tp")
    seq, chl = gate_b.shape
    rows, D = resid.shape
    cap = 4 * rows // S
    fh = w_gate.shape[2]
    B = S * cap
    G = 4 if S % 4 == 0 else 2
    Z = T // 2
    H = Z // 2
    vm = pl.BlockSpec(memory_space=pltpu.VMEM)
    hbm = pl.BlockSpec(memory_space=pl.ANY)
    dma = pltpu.SemaphoreType.DMA
    scratch = [
        pltpu.VMEM((chl, seq), BF16), pltpu.VMEM((chl, seq), BF16), pltpu.VMEM((chl, seq), BF16),
        pltpu.VMEM(w_out.shape, BF16), pltpu.VMEM((rows, D), BF16),
        pltpu.VMEM((fh, D), BF16), pltpu.VMEM((fh, D), BF16), pltpu.VMEM((fh, D), BF16),
        pltpu.VMEM((chl + 8, 128), F32), pltpu.VMEM((chl + 8, 128), F32),
        pltpu.VMEM((T, rows, 2 * chl), BF16), pltpu.VMEM((T, rows, 2 * chl), BF16),
        pltpu.VMEM((S, cap, D), BF16),
        pltpu.VMEM((T, B, D), BF16),
        pltpu.VMEM((Z, B, D), BF16), pltpu.VMEM((Z, B, D), BF16), pltpu.VMEM((Z, B, D), BF16),
        pltpu.VMEM((2, H, B, D), BF16),
        pltpu.VMEM((S, cap, D), BF16), pltpu.VMEM((B, D), BF16), pltpu.VMEM((rows, D), BF16),
        dma((8,)), dma((2,)), dma((T,)), dma((T,)), dma((S,)), dma((S,)),
        dma((2, H, G)), dma((2, H, G)), dma((Z, G)), dma((Z, G)), dma((Z,)), dma((Z,)),
        dma((2, H, G)), dma((2, H, G)), dma((S,)), dma((S,)),
    ]
    return pl.pallas_call(
        functools.partial(kernel, S, T, G),
        out_shape=jax.ShapeDtypeStruct((rows, D), BF16),
        in_specs=[hbm, hbm, hbm, vm, vm, hbm, hbm, vm, vm, vm, hbm, hbm, hbm],
        out_specs=vm,
        scratch_shapes=scratch,
        compiler_params=pltpu.CompilerParams(
            collective_id=0, has_side_effects=True, vmem_limit_bytes=60 * 1024 * 1024
        ),
    )(
        gate_b.T, gate_c.T, values_in.T, conv_w, documents.reshape(1, seq), w_out, resid,
        norm_gain.reshape(1, D), route_ids.T, route_weight.T,
        jnp.swapaxes(w_gate, 1, 2)[0], jnp.swapaxes(w_up, 1, 2)[0], w_down[0],
    )


def solution(mesh):
    return jax.shard_map(
        local,
        mesh=mesh,
        in_specs=(
            P("sp", "tp"), P("sp", "tp"), P("sp", "tp"), P(None, "tp"), P("sp"), P(),
            P(("sp", "tp"), None), P(), P(("sp", "tp"), None), P(("sp", "tp"), None),
            P("sp", None, "tp"), P("sp", None, "tp"), P("sp", "tp", None),
        ),
        out_specs=P(("sp", "tp"), None),
        check_vma=False,
    )
```
